512 devices in a mesh: grp: 2 (over y), sp: 64 (over z, core), tp: 4 (over x).
Axes of the slice: x: 4, y: 2, z: 32, core: 2. Of those that a mesh axis runs over, the one named last changes fastest.
The devices are a block of a 4x8x32 slice.
Arguments:
- tokens: bfloat16 [20480, 2048], P(('grp', 'sp')), parts along dimension 0, may hold values from -6 to 6
- norm_gain: float32 [2048], replicated, may hold values from 0.6 to 5
- query_weight: bfloat16 [2048, 2048], P('sp', 'tp')
- key_weight: bfloat16 [2048, 512], P('sp', 'tp')
- value_weight: bfloat16 [2048, 512], P('sp', 'tp'), may hold values from -0.125 to 0.125
- map_lambda: float32 [16], P('tp'), may hold values from 0.3 to 0.8
- head_gain: float32 [16, 128], P('tp'), may hold values from 0.1 to 1.9
- attn_out_weight: bfloat16 [2048, 2048], P('tp', 'sp'), may hold values from -0.125 to 0.125
- pool_out_weight: bfloat16 [2048, 2048], P('tp', 'sp'), may hold values from -0.09375 to 0.09375
Outputs:
- mixed_rows: bfloat16 [20480, 2048], P(('grp', 'sp', 'tp')), parts along dimension 0
- log_totals: float32 [2, 16, 20480], P(None, 'tp', ('grp', 'sp')), parts along dimension 2
The draws below stay inside these ranges and needn't reach their ends.
There are 2 independent parts, one for each index of `grp`. The reference program is written for one: setup_inputs(seed, part) draws one part's arguments, and reference() takes and returns one part's arrays. A program takes and returns all parts, laid end to end along the dimension named above; an argument that names none is the same for every part. Nothing has to cross between parts.
All inputs are finite; a program needn't handle non-finite values.
Results may differ from the reference program's by a relative error of at most 0.013.
The reference program's roundings to bfloat16 on the way (of `normed`, `head_rows` and `pooled`) count: a program that leaves them out, or rounds other values in their place, can miss the bound.
Values may be sent and summed in bfloat16 or wider, within the bound.
No kernel may reach another device: no remote copies, remote signals or barrier semaphores. Data moves between devices by JAX's collectives and lax.ppermute only.
A program may use at most 64 MiB of HBM per device.

```python
import math
import jax
import jax.numpy as jnp
from jax import lax

D = 2048
HEADS = 16
KV_HEADS = 4
HD = 64
VD = 128
SEQ = 10240


def projection_pair(key):
    base_key = jax.random.fold_in(key, 71)
    query_key, other_key = jax.random.split(base_key)
    spread_std = 1.32 / math.sqrt(D)
    w_query = jax.random.normal(query_key, (D, HEADS * 2 * HD), jnp.float32) * spread_std
    fresh_part = jax.random.normal(other_key, (D, KV_HEADS * 2 * HD), jnp.float32) * spread_std
    w_key = fresh_part
    return (w_query, w_key)


def draw_query_weight(key, part):
    return projection_pair(key)[0].astype(jnp.bfloat16)


def draw_key_weight(key, part):
    return projection_pair(key)[1].astype(jnp.bfloat16)


def draw_norm_gain(key, part):
    gain_key = jax.random.fold_in(key, 13)
    return jax.random.uniform(gain_key, (D,), jnp.float32, 0.6, 1.4)


def shard_levels(own_key, shape, cuts, least, top_value):
    level, own = 1.0, jax.random.fold_in(own_key, 6)
    for dim, shards_of in cuts:
        steps = jnp.exp(jax.random.uniform(jax.random.fold_in(own, dim), (shards_of,), jnp.float32, least / len(cuts), top_value / len(cuts)))
        level = level * jnp.repeat(steps, shape[dim] // shards_of).reshape([-1 if axis == dim else 1 for axis in range(len(shape))])
    return level


def scatter_about(stream_key, dims, deviation, limit, cuts=(), kind=jnp.bfloat16):
    values = deviation * jax.random.normal(stream_key, dims, jnp.float32)
    if cuts:
        values = values * shard_levels(stream_key, dims, cuts, -0.22, 0.18)
    return jnp.clip(values, -limit, limit).astype(kind)


def setup_inputs(seed: int = 0, part: int = 0) -> dict:
    streams_of = jax.random.split(jax.random.key(seed), 10)
    part_splits = jax.random.split(jax.random.fold_in(streams_of[9], part), 10)
    tokens = scatter_about(part_splits[0], (SEQ, D), 1.0, 6.0, ((0, 64),))
    norm_gain = draw_norm_gain(jax.random.fold_in(streams_of[9], 71), part)
    query_weight = draw_query_weight(jax.random.fold_in(streams_of[9], 71), part)
    key_weight = draw_key_weight(jax.random.fold_in(streams_of[9], 71), part)
    value_weight = scatter_about(streams_of[4], (D, KV_HEADS * VD), D ** -0.5, 0.125, ((0, 64), (1, 4)))
    map_lambda = jnp.clip(0.3 + 0.5 * jax.random.uniform(streams_of[5], (HEADS,), jnp.float32) ** shard_levels(streams_of[5], (HEADS,), ((0, 4),), -0.2, 0.2), 0.3, 0.8)
    head_gain = jnp.clip(1.0 + 0.18 * jax.random.normal(streams_of[6], (HEADS, VD), jnp.float32), 0.1, 1.9)
    attn_out_weight = scatter_about(streams_of[7], (HEADS * VD, D), (HEADS * VD) ** -0.5, 0.125, ((0, 4), (1, 64)))
    pool_out_weight = scatter_about(streams_of[8], (D, D), (2 * D) ** -0.5, 0.09375, ((0, 4), (1, 64)))
    return {"tokens": tokens, "norm_gain": norm_gain, "query_weight": query_weight, "key_weight": key_weight, "value_weight": value_weight, "map_lambda": map_lambda, "head_gain": head_gain, "attn_out_weight": attn_out_weight, "pool_out_weight": pool_out_weight}


epsilon = 1e-06

def reference(tokens, norm_gain, query_weight, key_weight, value_weight, map_lambda, head_gain, attn_out_weight, pool_out_weight):
    group_heads = HEADS // KV_HEADS
    tokens_wide = tokens.astype(jnp.float32)
    normed = (tokens_wide * lax.rsqrt(lax.optimization_barrier(jnp.mean(tokens_wide * tokens_wide, axis=-1, keepdims=True)) + epsilon) * norm_gain).astype(jnp.bfloat16)
    queries = jnp.dot(normed, query_weight, preferred_element_type=jnp.float32).astype(jnp.bfloat16)
    keys = jnp.dot(normed, key_weight, preferred_element_type=jnp.float32).astype(jnp.bfloat16)
    values = jnp.dot(normed, value_weight, preferred_element_type=jnp.float32).astype(jnp.bfloat16)
    keys_f32 = keys.reshape(SEQ, KV_HEADS, 2, HD).astype(jnp.float32)
    values_f32 = values.reshape(SEQ, KV_HEADS, VD).astype(jnp.float32)
    block_len = math.gcd(SEQ, 256)
    query_blocks = queries.reshape(SEQ // block_len, block_len, KV_HEADS, group_heads, 2, HD)
    lambdas = map_lambda.reshape(KV_HEADS, group_heads, 1, 1)
    gains = head_gain.reshape(KV_HEADS, group_heads, 1, VD)

    def attend(query_blk):
        scores = jnp.einsum('qhgmd,khmd->hgmqk', query_blk.astype(jnp.float32), keys_f32) * HD ** (-0.5)
        highest = lax.optimization_barrier(jnp.max(scores, axis=-1))
        weights = jnp.exp(scores - highest[..., None])
        totals = lax.optimization_barrier(jnp.sum(weights, axis=-1))
        weights_b = lax.optimization_barrier(weights.astype(jnp.bfloat16)).astype(jnp.float32)
        reads = jnp.einsum('hgmqk,khe->hgmqe', weights_b, values_f32) / totals[..., None]
        contrast = reads[:, :, 0] - lambdas * reads[:, :, 1]
        scaled = contrast * lax.rsqrt(lax.optimization_barrier(jnp.mean(contrast * contrast, axis=-1, keepdims=True)) + epsilon) * gains
        head_rows = jnp.transpose(scaled, (2, 0, 1, 3)).reshape(block_len, HEADS * VD)
        return (head_rows.astype(jnp.bfloat16), highest + jnp.log(totals))
    head_rows, log_parts = lax.map(attend, query_blocks)
    head_rows = head_rows.reshape(SEQ, HEADS * VD)
    log_totals = jnp.transpose(log_parts, (3, 1, 2, 0, 4)).reshape(2, HEADS, SEQ)
    normed_f32 = normed.astype(jnp.float32)
    prefix = jnp.concatenate([jnp.zeros((1, D), jnp.float32), jnp.cumsum(normed_f32, axis=0)], axis=0)
    position = jnp.arange(SEQ)
    group_width = D // 4
    pieces = []
    for group in range(4):
        window = 2 ** (group + 1)
        lower_edge = jnp.clip(position - window // 2, 0, SEQ)
        upper_edge = jnp.clip(position + window - window // 2, 0, SEQ)
        counts_f = (upper_edge - lower_edge).astype(jnp.float32)[:, None]
        columns = prefix[:, group * group_width:(group + 1) * group_width]
        own_chan = normed_f32[:, group * group_width:(group + 1) * group_width]
        pieces.append((columns[upper_edge] - columns[lower_edge]) / counts_f - own_chan)
    pooled = jnp.concatenate(pieces, axis=1).astype(jnp.bfloat16)
    mixed = jnp.dot(head_rows, attn_out_weight, preferred_element_type=jnp.float32) + jnp.dot(pooled, pool_out_weight, preferred_element_type=jnp.float32)
    return (mixed.astype(jnp.bfloat16), log_totals)
```

```python
import functools
import math

import jax
import jax.numpy as jnp
from jax import lax
from jax.experimental import pallas as pl
from jax.experimental.pallas import tpu as pltpu
from jax.sharding import Mesh, PartitionSpec as P

HD = 64
VD = 128
POOL_SPAN = 16
CORES = 2
epsilon = 1e-06
LOG2E = math.log2(math.e)
CHUNK = 1280
TILE = 256
SP = ("zh", "zm", "zl", "core")
Z = ("zh", "zm", "zl")
SWAP = [(0, 1), (1, 0)]


def mixer_kernel(counts, place_ref, x_ref, pooled_ref, gain_ref, lam_ref, *refs):
    late_count, kv_count = counts
    late, refs = refs[:late_count], refs[late_count:]
    mine, refs = refs[:kv_count], refs[kv_count:]
    other, refs = refs[:kv_count], refs[kv_count:]
    out_ref, lse_ref, qT, qrows, m_s, l_s, acc, k_all, v_all, rows_s = refs
    n = x_ref.shape[0]
    width = pooled_ref.shape[1]
    heads = width // VD
    half = heads * n
    tiles = 2 * half // TILE

    def fill(keys, values):
        at = 0
        for k, v in zip(keys, values):
            k_all[at : at + k.shape[0], :] = k[...]
            v_all[at : at + v.shape[0], :] = v[...]
            at += k.shape[0]

    @pl.when(place_ref[0] == 0)
    def _():
        fill(mine, other)

    @pl.when(place_ref[0] != 0)
    def _():
        fill(other, mine)

    spots = []
    at, slot = 0, 0
    for w in late:
        spots.append((place_ref[1 + slot], at, w))
        at += w.shape[0]
        if at == x_ref.shape[1] // 4:
            at, slot = 0, slot + 1
    set_width = x_ref.shape[1] // 4

    def columns(where, at, count):
        return pl.ds(pl.multiple_of(where * set_width + at, 128), count)

    queries = jnp.zeros((n, width), jnp.float32)
    for where, at, w in spots:
        queries += jnp.dot(
            x_ref[:, columns(where, at, w.shape[0])], w[:, :width], preferred_element_type=jnp.float32
        )
    queries = queries.astype(jnp.bfloat16).astype(jnp.float32) * (HD**-0.5 * LOG2E)
    lane = lax.broadcasted_iota(jnp.int32, (n, VD), 1)
    for g in range(heads):
        for m in range(2):
            part = jnp.where((lane < HD) == (m == 0), queries[:, g * VD : (g + 1) * VD], 0.0)
            hi = part.astype(jnp.bfloat16)
            lo = (part - hi.astype(jnp.float32)).astype(jnp.bfloat16)
            row = m * half + g * n
            qrows[row : row + n, :VD] = hi
            qrows[row : row + n, VD:] = lo
    for j in range(tiles):
        qT[:, j * TILE : (j + 1) * TILE] = qrows[j * TILE : (j + 1) * TILE, :].T
    m_s[...] = jnp.full(m_s.shape, -jnp.inf, jnp.float32)
    l_s[...] = jnp.zeros_like(l_s)
    acc[...] = jnp.zeros_like(acc)

    def block(i, carry):
        rows = pl.ds(pl.multiple_of(i * CHUNK, CHUNK), CHUNK)
        keys = k_all[rows, :]
        both = jnp.concatenate([keys, keys], axis=1)
        values_t = v_all[rows, :].T
        scores, weights = {}, {}

        def score(j):
            scores[j] = jnp.dot(
                both, qT[:, j * TILE : (j + 1) * TILE], preferred_element_type=jnp.float32
            )

        def soften(j):
            cols = slice(j * TILE, (j + 1) * TILE)
            s = scores.pop(j)
            m_old = m_s[:, cols]
            m_new = jnp.maximum(m_old, jnp.max(s, axis=0, keepdims=True))
            p = jnp.exp2(s - m_new)
            alpha = jnp.exp2(m_old - m_new)
            m_s[:, cols] = m_new
            l_s[:, cols] = l_s[:, cols] * alpha + jnp.sum(p, axis=0, keepdims=True)
            weights[j] = (alpha, p.astype(jnp.bfloat16))

        def mix(j):
            cols = slice(j * TILE, (j + 1) * TILE)
            alpha, p = weights.pop(j)
            acc[:, cols] = acc[:, cols] * alpha + jnp.dot(
                values_t, p, preferred_element_type=jnp.float32
            )

        for t in range(tiles + 2):
            if t < tiles:
                score(t)
            if 1 <= t <= tiles:
                soften(t - 1)
            if t >= 2:
                mix(t - 2)
        return carry

    lax.fori_loop(0, k_all.shape[0] // CHUNK, block, 0)

    totals = l_s[...]
    lse_ref[...] = m_s[...] * (1.0 / LOG2E) + jnp.log(totals)
    reads = acc[...] / totals
    contrast = reads[:, :half] - lam_ref[...] * reads[:, half:]
    scaled = contrast * lax.rsqrt(jnp.mean(contrast * contrast, axis=0, keepdims=True) + epsilon)
    rows = scaled.T
    for g in range(heads):
        rows_s[:, g * VD : (g + 1) * VD] = (
            rows[g * n : (g + 1) * n, :] * gain_ref[g : g + 1, :]
        ).astype(jnp.bfloat16)
    rows_s[:, width:] = pooled_ref[...]
    sources = rows_s[...]
    for where, at, w in spots:
        out_ref[:, columns(where, at, w.shape[0])] = lax.dot_general(
            sources, w[:, width:], (((1,), (1,)), ((), ())), preferred_element_type=jnp.float32
        ).astype(jnp.bfloat16)


def mixer(place, x, pooled, gain, lam, late, mine, other):
    n, model = x.shape
    width = pooled.shape[1]
    heads = width // VD
    cols = 2 * heads * n
    keys = sum(p.shape[0] for p in mine)
    vmem = pl.BlockSpec(memory_space=pltpu.VMEM)
    return pl.pallas_call(
        functools.partial(mixer_kernel, (len(late), len(mine))),
        out_shape=(
            jax.ShapeDtypeStruct((n, model), jnp.bfloat16),
            jax.ShapeDtypeStruct((1, cols), jnp.float32),
        ),
        in_specs=[pl.BlockSpec(memory_space=pltpu.SMEM)] + [vmem] * (4 + len(late) + 2 * len(mine)),
        out_specs=(vmem, vmem),
        scratch_shapes=[
            pltpu.VMEM((2 * VD, cols), jnp.bfloat16),
            pltpu.VMEM((cols, 2 * VD), jnp.bfloat16),
            pltpu.VMEM((1, cols), jnp.float32),
            pltpu.VMEM((1, cols), jnp.float32),
            pltpu.VMEM((VD, cols), jnp.float32),
            pltpu.VMEM((keys, VD), jnp.bfloat16),
            pltpu.VMEM((keys, VD), jnp.bfloat16),
            pltpu.VMEM((n, 2 * width), jnp.bfloat16),
        ],
        cost_estimate=pl.CostEstimate(
            flops=2 * cols * keys * 3 * VD, bytes_accessed=keys * 4 * VD, transcendentals=cols * keys
        ),
        name="mixer",
    )(place, x, pooled, gain, jnp.repeat(lam, n)[None, :], *late, *mine, *other)


def spread(x, axis):
    count = lax.axis_size(axis)
    return lax.all_to_all(jnp.broadcast_to(x[None], (count, *x.shape)), axis, 0, 0, tiled=True)


def shifted(x, axis, by):
    count = lax.axis_size(axis)
    return lax.ppermute(x, axis, [((i + by) % count, i) for i in range(count)])


def partner(x):
    return lax.ppermute(x, "core", SWAP)


def pooled_rows(normed, tp_index, sp_index, sp_count, group_width):
    rows = normed.shape[0]
    reach = POOL_SPAN // 2
    own = lax.dynamic_slice_in_dim(normed, tp_index * group_width, group_width, 1)
    ends = sp_count - 1
    before = lax.ppermute(own[rows - reach :], SP, [(i, i + 1) for i in range(ends)])
    after = lax.ppermute(own[:reach], SP, [(i + 1, i) for i in range(ends)])
    padded = jnp.concatenate([before, own, after], axis=0)
    window = jnp.left_shift(jnp.int32(2), tp_index)
    half = window // 2
    row = lax.broadcasted_iota(jnp.int32, (rows, rows + 2 * reach), 0)
    col = lax.broadcasted_iota(jnp.int32, (rows, rows + 2 * reach), 1) - reach
    band = ((col >= row - half) & (col < row + window - half)).astype(jnp.bfloat16)
    sums = jnp.dot(band, padded, preferred_element_type=jnp.float32)
    seq_len = rows * sp_count
    position = sp_index * rows + jnp.arange(rows, dtype=jnp.int32)
    lower = jnp.clip(position - half, 0, seq_len)
    upper = jnp.clip(position + window - half, 0, seq_len)
    counts = (upper - lower).astype(jnp.float32)[:, None]
    return (sums / counts - own.astype(jnp.float32)).astype(jnp.bfloat16)


def regrouped(x, outer, inner):
    rows, model = x.shape
    return jnp.swapaxes(x.reshape(rows, outer, inner, -1), 1, 2).reshape(rows, model)


def on_device(tokens, norm_gain, wq, wk, wv, map_lambda, head_gain, ao, po):
    zh, zm, zl = (lax.axis_size(a) for a in Z)
    sp_count = zh * zm * zl * CORES
    sp_index, tp_index = lax.axis_index(SP), lax.axis_index("tp")
    near, core = lax.axis_index("zl"), lax.axis_index("core")
    rows, model = tokens.shape
    local_heads = map_lambda.shape[0]
    group_width = po.shape[0]

    held = lax.all_gather(
        jnp.concatenate([wq, ao.T, po.T], axis=1), ("zh", "zm"), axis=0, tiled=True
    )

    wide = tokens.astype(jnp.float32)
    normed = (
        wide * lax.rsqrt(jnp.mean(wide * wide, axis=-1, keepdims=True) + epsilon) * norm_gain
    ).astype(jnp.bfloat16)
    beside = partner(normed)

    pair = lax.all_to_all(jnp.stack([wk, wv]), "core", 0, 0, tiled=True).reshape(-1, wk.shape[1])
    far = spread(pair, "zh")
    whole = jnp.swapaxes(spread(far, ("zm", "zl")), 0, 1).reshape(model, -1)

    def project(x):
        return jnp.dot(x, whole, preferred_element_type=jnp.float32).astype(jnp.bfloat16)

    ours, theirs = project(normed), project(beside)
    first = jnp.where(core == 0, ours, theirs)
    second = jnp.where(core == 0, theirs, ours)
    own = lax.all_gather(jnp.concatenate([first, second], axis=0), "zh", axis=0, tiled=True)
    mid = own.shape[0] // 2
    mine = [
        own,
        shifted(own, Z, 1),
        shifted(own, Z, -1),
        shifted(own[:mid], Z, 2),
        shifted(own[mid:], Z, -2),
    ]
    other = [partner(p) for p in mine]

    cut = held.shape[0] // 2
    beyond = [shifted(held[:cut], Z, 1), shifted(held[cut:], Z, -1)]
    late = [held, partner(held), *beyond, *(partner(p) for p in beyond)]
    slots = [2 * near + core, 2 * near + 1 - core, 2 * (1 - near) + core, 2 * (1 - near) + 1 - core]
    place = jnp.stack([core, *slots]).astype(jnp.int32)

    pooled = pooled_rows(normed, tp_index, sp_index, sp_count, group_width)
    partial, lse = mixer(
        place,
        regrouped(normed, zh * zm, zl * CORES),
        pooled,
        head_gain,
        map_lambda,
        late,
        mine,
        other,
    )
    log_totals = lse.reshape(2, local_heads, rows)
    tp = lax.axis_size("tp")
    arrived = lax.all_to_all(
        partial.reshape(tp, rows // tp, -1), "tp", split_axis=0, concat_axis=0, tiled=True
    )
    mixed = arrived.astype(jnp.float32).sum(axis=0).astype(jnp.bfloat16)
    return regrouped(mixed, zl * CORES, zh * zm), log_totals


def solution(mesh):
    grp, sp, tp = (mesh.shape[a] for a in ("grp", "sp", "tp"))
    fine = Mesh(
        mesh.devices.reshape(grp, sp // (4 * CORES), 2, 2, CORES, tp), ("grp", *SP, "tp")
    )
    placed = (
        P(("grp", *SP), None),
        P(),
        P(SP, "tp"),
        P(SP, "tp"),
        P(SP, "tp"),
        P("tp"),
        P("tp", None),
        P("tp", SP),
        P("tp", SP),
    )
    return jax.shard_map(
        on_device,
        mesh=fine,
        in_specs=placed,
        out_specs=(P(("grp", *SP, "tp"), None), P(None, "tp", ("grp", *SP))),
        check_vma=False,
    )
```

```python
import functools
import math

import jax
import jax.numpy as jnp
from jax import lax
from jax.experimental import pallas as pl
from jax.experimental.pallas import tpu as pltpu
from jax.sharding import Mesh, PartitionSpec as P

HD = 64
VD = 128
POOL_SPAN = 16
CORES = 2
epsilon = 1e-06
LOG2E = math.log2(math.e)
CHUNK = 1280
TILE = 256
SP = ("zh", "zm", "zl", "core")
Z = ("zh", "zm", "zl")
SWAP = [(0, 1), (1, 0)]


def attention_kernel(kv_count, place_ref, q_ref, gain_ref, lam_ref, *refs):
    mine, refs = refs[:kv_count], refs[kv_count:]
    other, refs = refs[:kv_count], refs[kv_count:]
    rows_ref, lse_ref, qT, qrows, m_s, l_s, acc, k_all, v_all = refs
    n, width = q_ref.shape
    heads = width // VD
    half = heads * n
    tiles = 2 * half // TILE

    def fill(keys, values):
        at = 0
        for k, v in zip(keys, values):
            k_all[at : at + k.shape[0], :] = k[...]
            v_all[at : at + v.shape[0], :] = v[...]
            at += k.shape[0]

    @pl.when(place_ref[0] == 0)
    def _():
        fill(mine, other)

    @pl.when(place_ref[0] != 0)
    def _():
        fill(other, mine)

    queries = q_ref[...].astype(jnp.float32) * (HD**-0.5 * LOG2E)
    lane = lax.broadcasted_iota(jnp.int32, (n, VD), 1)
    for g in range(heads):
        for m in range(2):
            part = jnp.where((lane < HD) == (m == 0), queries[:, g * VD : (g + 1) * VD], 0.0)
            hi = part.astype(jnp.bfloat16)
            lo = (part - hi.astype(jnp.float32)).astype(jnp.bfloat16)
            row = m * half + g * n
            qrows[row : row + n, :VD] = hi
            qrows[row : row + n, VD:] = lo
    for j in range(tiles):
        qT[:, j * TILE : (j + 1) * TILE] = qrows[j * TILE : (j + 1) * TILE, :].T
    m_s[...] = jnp.full(m_s.shape, -jnp.inf, jnp.float32)
    l_s[...] = jnp.zeros_like(l_s)
    acc[...] = jnp.zeros_like(acc)

    def block(i, carry):
        rows = pl.ds(pl.multiple_of(i * CHUNK, CHUNK), CHUNK)
        keys = k_all[rows, :]
        both = jnp.concatenate([keys, keys], axis=1)
        values_t = v_all[rows, :].T
        scores, weights = {}, {}

        def score(j):
            scores[j] = jnp.dot(
                both, qT[:, j * TILE : (j + 1) * TILE], preferred_element_type=jnp.float32
            )

        def soften(j):
            cols = slice(j * TILE, (j + 1) * TILE)
            s = scores.pop(j)
            m_old = m_s[:, cols]
            m_new = jnp.maximum(m_old, jnp.max(s, axis=0, keepdims=True))
            p = jnp.exp2(s - m_new)
            alpha = jnp.exp2(m_old - m_new)
            m_s[:, cols] = m_new
            l_s[:, cols] = l_s[:, cols] * alpha + jnp.sum(p, axis=0, keepdims=True)
            weights[j] = (alpha, p.astype(jnp.bfloat16))

        def mix(j):
            cols = slice(j * TILE, (j + 1) * TILE)
            alpha, p = weights.pop(j)
            acc[:, cols] = acc[:, cols] * alpha + jnp.dot(
                values_t, p, preferred_element_type=jnp.float32
            )

        for t in range(tiles + 2):
            if t < tiles:
                score(t)
            if 1 <= t <= tiles:
                soften(t - 1)
            if t >= 2:
                mix(t - 2)
        return carry

    lax.fori_loop(0, k_all.shape[0] // CHUNK, block, 0)

    totals = l_s[...]
    lse_ref[...] = m_s[...] * (1.0 / LOG2E) + jnp.log(totals)
    reads = acc[...] / totals
    contrast = reads[:, :half] - lam_ref[...] * reads[:, half:]
    scaled = contrast * lax.rsqrt(jnp.mean(contrast * contrast, axis=0, keepdims=True) + epsilon)
    rows = scaled.T
    for g in range(heads):
        rows_ref[:, g * VD : (g + 1) * VD] = (
            rows[g * n : (g + 1) * n, :] * gain_ref[g : g + 1, :]
        ).astype(jnp.bfloat16)


def attend(place, queries, gain, lam, mine, other):
    n, width = queries.shape
    cols = 2 * (width // VD) * n
    keys = sum(p.shape[0] for p in mine)
    vmem = pl.BlockSpec(memory_space=pltpu.VMEM)
    return pl.pallas_call(
        functools.partial(attention_kernel, len(mine)),
        out_shape=(
            jax.ShapeDtypeStruct((n, width), jnp.bfloat16),
            jax.ShapeDtypeStruct((1, cols), jnp.float32),
        ),
        in_specs=[pl.BlockSpec(memory_space=pltpu.SMEM)] + [vmem] * (3 + 2 * len(mine)),
        out_specs=(vmem, vmem),
        scratch_shapes=[
            pltpu.VMEM((2 * VD, cols), jnp.bfloat16),
            pltpu.VMEM((cols, 2 * VD), jnp.bfloat16),
            pltpu.VMEM((1, cols), jnp.float32),
            pltpu.VMEM((1, cols), jnp.float32),
            pltpu.VMEM((VD, cols), jnp.float32),
            pltpu.VMEM((keys, VD), jnp.bfloat16),
            pltpu.VMEM((keys, VD), jnp.bfloat16),
        ],
        cost_estimate=pl.CostEstimate(
            flops=2 * cols * keys * 3 * VD, bytes_accessed=keys * 4 * VD, transcendentals=cols * keys
        ),
        name="attention",
    )(place, queries, gain, jnp.repeat(lam, n)[None, :], *mine, *other)


def spread(x, axis):
    count = lax.axis_size(axis)
    return lax.all_to_all(jnp.broadcast_to(x[None], (count, *x.shape)), axis, 0, 0, tiled=True)


def shifted(x, axis, by):
    count = lax.axis_size(axis)
    return lax.ppermute(x, axis, [((i + by) % count, i) for i in range(count)])


def partner(x):
    return lax.ppermute(x, "core", SWAP)


def halo(own):
    reach = POOL_SPAN // 2
    ends = math.prod(lax.axis_size(a) for a in SP) - 1
    before = lax.ppermute(own[own.shape[0] - reach :], SP, [(i, i + 1) for i in range(ends)])
    after = lax.ppermute(own[:reach], SP, [(i + 1, i) for i in range(ends)])
    return before, after


def pooled_rows(own, before, after, tp_index, sp_index, sp_count):
    rows = own.shape[0]
    reach = POOL_SPAN // 2
    padded = jnp.concatenate([before, own, after], axis=0)
    window = jnp.left_shift(jnp.int32(2), tp_index)
    half = window // 2
    row = lax.broadcasted_iota(jnp.int32, (rows, rows + 2 * reach), 0)
    col = lax.broadcasted_iota(jnp.int32, (rows, rows + 2 * reach), 1) - reach
    band = ((col >= row - half) & (col < row + window - half)).astype(jnp.bfloat16)
    sums = jnp.dot(band, padded, preferred_element_type=jnp.float32)
    seq_len = rows * sp_count
    position = sp_index * rows + jnp.arange(rows, dtype=jnp.int32)
    lower = jnp.clip(position - half, 0, seq_len)
    upper = jnp.clip(position + window - half, 0, seq_len)
    counts = (upper - lower).astype(jnp.float32)[:, None]
    return (sums / counts - own.astype(jnp.float32)).astype(jnp.bfloat16)


def on_device(tokens, norm_gain, wq, wk, wv, map_lambda, head_gain, ao, po):
    zh, zm, zl = (lax.axis_size(a) for a in Z)
    sp_count = zh * zm * zl * CORES
    sp_index, tp_index = lax.axis_index(SP), lax.axis_index("tp")
    core = lax.axis_index("core")
    rows, model = tokens.shape
    local_heads = map_lambda.shape[0]
    group_width = po.shape[0]

    late = jnp.concatenate([wq, ao.T, po.T], axis=1)
    late, wk, wv = lax.optimization_barrier((late, wk, wv))
    late = lax.all_gather(late, SP, axis=0, tiled=True)

    wide = tokens.astype(jnp.float32)
    normed = (
        wide * lax.rsqrt(jnp.mean(wide * wide, axis=-1, keepdims=True) + epsilon) * norm_gain
    ).astype(jnp.bfloat16)
    own_chan = lax.dynamic_slice_in_dim(normed, tp_index * group_width, group_width, 1)
    beside = partner(normed)
    before, after = halo(own_chan)

    pair = lax.all_to_all(jnp.stack([wk, wv]), "core", 0, 0, tiled=True).reshape(-1, wk.shape[1])
    far = spread(pair, "zh")
    far, beside, before, after = lax.optimization_barrier((far, beside, before, after))
    whole = jnp.swapaxes(spread(far, ("zm", "zl")), 0, 1).reshape(model, -1)

    def project(x):
        return jnp.dot(x, whole, preferred_element_type=jnp.float32).astype(jnp.bfloat16)

    ours, theirs = project(normed), project(beside)
    first = jnp.where(core == 0, ours, theirs)
    second = jnp.where(core == 0, theirs, ours)
    own = lax.all_gather(jnp.concatenate([first, second], axis=0), "zh", axis=0, tiled=True)
    mid = own.shape[0] // 2
    mine = [
        own,
        shifted(own, Z, 1),
        shifted(own, Z, -1),
        shifted(own[:mid], Z, 2),
        shifted(own[mid:], Z, -2),
    ]
    other = [partner(p) for p in mine]

    pooled = pooled_rows(own_chan, before, after, tp_index, sp_index, sp_count)

    late, other[-1] = lax.optimization_barrier((late, other[-1]))
    width = wq.shape[1]
    queries = jnp.dot(
        normed, late[:, :width], preferred_element_type=jnp.float32
    ).astype(jnp.bfloat16)
    head_rows, lse = attend(core.reshape(1), queries, head_gain, map_lambda, mine, other)
    log_totals = lse.reshape(2, local_heads, rows)
    partial = lax.dot_general(
        jnp.concatenate([head_rows, pooled], axis=1),
        late[:, width:],
        (((1,), (1,)), ((), ())),
        preferred_element_type=jnp.float32,
    ).astype(jnp.bfloat16)
    tp = lax.axis_size("tp")
    arrived = lax.all_to_all(
        partial.reshape(tp, rows // tp, -1), "tp", split_axis=0, concat_axis=0, tiled=True
    )
    return arrived.astype(jnp.float32).sum(axis=0).astype(jnp.bfloat16), log_totals


def solution(mesh):
    grp, sp, tp = (mesh.shape[a] for a in ("grp", "sp", "tp"))
    fine = Mesh(
        mesh.devices.reshape(grp, sp // (4 * CORES), 2, 2, CORES, tp), ("grp", *SP, "tp")
    )
    placed = (
        P(("grp", *SP), None),
        P(),
        P(SP, "tp"),
        P(SP, "tp"),
        P(SP, "tp"),
        P("tp"),
        P("tp", None),
        P("tp", SP),
        P("tp", SP),
    )
    return jax.shard_map(
        on_device,
        mesh=fine,
        in_specs=placed,
        out_specs=(P(("grp", *SP, "tp"), None), P(None, "tp", ("grp", *SP))),
        check_vma=False,
    )
```

```python
import functools
import math

import jax
import jax.numpy as jnp
from jax import lax
from jax.experimental import pallas as pl
from jax.experimental.pallas import tpu as pltpu
from jax.sharding import Mesh, PartitionSpec as P

HD = 64
VD = 128
POOL_SPAN = 16
CORES = 2
epsilon = 1e-06
LOG2E = math.log2(math.e)
CHUNK = 2560
TILE = 256
ONES = 16
SP = ("zh", "zm", "zl", "core")
Z = ("zh", "zm", "zl")
SWAP = [(0, 1), (1, 0)]


def attention_kernel(kv_count, place_ref, q_ref, gain_ref, lam_ref, *refs):
    mine, refs = refs[:kv_count], refs[kv_count:]
    other, refs = refs[:kv_count], refs[kv_count:]
    rows_ref, lse_ref, qT, qrows, m_s, acc, k_all, v_all = refs
    n, width = q_ref.shape
    heads = width // VD
    half = heads * n
    tiles = 2 * half // TILE

    def fill(keys, values):
        at = 0
        for k, v in zip(keys, values):
            k_all[at : at + k.shape[0], :] = k[...]
            v_all[at : at + v.shape[0], :] = v[...]
            at += k.shape[0]

    @pl.when(place_ref[0] == 0)
    def _():
        fill(mine, other)

    @pl.when(place_ref[0] != 0)
    def _():
        fill(other, mine)

    queries = q_ref[...].astype(jnp.float32) * (HD**-0.5 * LOG2E)
    lane = lax.broadcasted_iota(jnp.int32, (n, VD), 1)
    for g in range(heads):
        for m in range(2):
            part = jnp.where((lane < HD) == (m == 0), queries[:, g * VD : (g + 1) * VD], 0.0)
            hi = part.astype(jnp.bfloat16)
            lo = (part - hi.astype(jnp.float32)).astype(jnp.bfloat16)
            row = m * half + g * n
            qrows[row : row + n, :VD] = hi
            qrows[row : row + n, VD:] = lo
    for j in range(tiles):
        qT[:, j * TILE : (j + 1) * TILE] = qrows[j * TILE : (j + 1) * TILE, :].T
    m_s[...] = jnp.full(m_s.shape, -jnp.inf, jnp.float32)
    acc[...] = jnp.zeros_like(acc)

    def block(i, carry):
        rows = pl.ds(pl.multiple_of(i * CHUNK, CHUNK), CHUNK)
        keys = k_all[rows, :]
        both = jnp.concatenate([keys, keys], axis=1)
        values_t = jnp.concatenate(
            [v_all[rows, :].T, jnp.ones((ONES, CHUNK), jnp.bfloat16)], axis=0
        )
        scores, weights = {}, {}

        def score(j):
            scores[j] = jnp.dot(
                both, qT[:, j * TILE : (j + 1) * TILE], preferred_element_type=jnp.float32
            )

        def soften(j):
            cols = slice(j * TILE, (j + 1) * TILE)
            s = scores.pop(j)
            m_old = m_s[:, cols]
            m_new = jnp.maximum(m_old, jnp.max(s, axis=0, keepdims=True))
            p = jnp.exp2(s - m_new)
            alpha = jnp.exp2(m_old - m_new)
            m_s[:, cols] = m_new
            weights[j] = (alpha, p.astype(jnp.bfloat16))

        def mix(j):
            cols = slice(j * TILE, (j + 1) * TILE)
            alpha, p = weights.pop(j)
            acc[:, cols] = acc[:, cols] * alpha + jnp.dot(
                values_t, p, preferred_element_type=jnp.float32
            )

        for t in range(tiles + 3):
            if t < tiles:
                score(t)
            if 1 <= t <= tiles:
                soften(t - 1)
            if t >= 3:
                mix(t - 3)
        return carry

    lax.fori_loop(0, k_all.shape[0] // CHUNK, block, 0)

    totals = acc[VD : VD + 1, :]
    lse_ref[...] = m_s[...] * (1.0 / LOG2E) + jnp.log(totals)
    reads = acc[:VD, :] / totals
    contrast = reads[:, :half] - lam_ref[...] * reads[:, half:]
    scaled = contrast * lax.rsqrt(jnp.mean(contrast * contrast, axis=0, keepdims=True) + epsilon)
    rows = scaled.T
    for g in range(heads):
        rows_ref[:, g * VD : (g + 1) * VD] = (
            rows[g * n : (g + 1) * n, :] * gain_ref[g : g + 1, :]
        ).astype(jnp.bfloat16)


def attend(place, queries, gain, lam, mine, other):
    n, width = queries.shape
    cols = 2 * (width // VD) * n
    keys = sum(p.shape[0] for p in mine)
    vmem = pl.BlockSpec(memory_space=pltpu.VMEM)
    return pl.pallas_call(
        functools.partial(attention_kernel, len(mine)),
        out_shape=(
            jax.ShapeDtypeStruct((n, width), jnp.bfloat16),
            jax.ShapeDtypeStruct((1, cols), jnp.float32),
        ),
        in_specs=[pl.BlockSpec(memory_space=pltpu.SMEM)] + [vmem] * (3 + 2 * len(mine)),
        out_specs=(vmem, vmem),
        scratch_shapes=[
            pltpu.VMEM((2 * VD, cols), jnp.bfloat16),
            pltpu.VMEM((cols, 2 * VD), jnp.bfloat16),
            pltpu.VMEM((1, cols), jnp.float32),
            pltpu.VMEM((VD + ONES, cols), jnp.float32),
            pltpu.VMEM((keys, VD), jnp.bfloat16),
            pltpu.VMEM((keys, VD), jnp.bfloat16),
        ],
        cost_estimate=pl.CostEstimate(
            flops=2 * cols * keys * 3 * VD, bytes_accessed=keys * 4 * VD, transcendentals=cols * keys
        ),
        name="attention",
    )(place, queries, gain, jnp.repeat(lam, n)[None, :], *mine, *other)


def spread(x, axis):
    count = lax.axis_size(axis)
    return lax.all_to_all(jnp.broadcast_to(x[None], (count, *x.shape)), axis, 0, 0, tiled=True)


def shifted(x, axis, by):
    count = lax.axis_size(axis)
    return lax.ppermute(x, axis, [((i + by) % count, i) for i in range(count)])


def partner(x):
    return lax.ppermute(x, "core", SWAP)


def halo(own):
    reach = POOL_SPAN // 2
    ends = math.prod(lax.axis_size(a) for a in SP) - 1
    before = lax.ppermute(own[own.shape[0] - reach :], SP, [(i, i + 1) for i in range(ends)])
    after = lax.ppermute(own[:reach], SP, [(i + 1, i) for i in range(ends)])
    return before, after


def pooled_rows(own, before, after, tp_index, sp_index, sp_count):
    rows = own.shape[0]
    reach = POOL_SPAN // 2
    padded = jnp.concatenate([before, own, after], axis=0)
    window = jnp.left_shift(jnp.int32(2), tp_index)
    half = window // 2
    row = lax.broadcasted_iota(jnp.int32, (rows, rows + 2 * reach), 0)
    col = lax.broadcasted_iota(jnp.int32, (rows, rows + 2 * reach), 1) - reach
    band = ((col >= row - half) & (col < row + window - half)).astype(jnp.bfloat16)
    sums = jnp.dot(band, padded, preferred_element_type=jnp.float32)
    seq_len = rows * sp_count
    position = sp_index * rows + jnp.arange(rows, dtype=jnp.int32)
    lower = jnp.clip(position - half, 0, seq_len)
    upper = jnp.clip(position + window - half, 0, seq_len)
    counts = (upper - lower).astype(jnp.float32)[:, None]
    return (sums / counts - own.astype(jnp.float32)).astype(jnp.bfloat16)


def on_device(tokens, norm_gain, wq, wk, wv, map_lambda, head_gain, ao, po):
    zh, zm, zl = (lax.axis_size(a) for a in Z)
    sp_count = zh * zm * zl * CORES
    sp_index, tp_index = lax.axis_index(SP), lax.axis_index("tp")
    core = lax.axis_index("core")
    rows, model = tokens.shape
    local_heads = map_lambda.shape[0]
    group_width = po.shape[0]

    late = jnp.concatenate([wq, ao.T, po.T], axis=1)
    late, wk, wv = lax.optimization_barrier((late, wk, wv))
    late = lax.all_gather(late, SP, axis=0, tiled=True)

    wide = tokens.astype(jnp.float32)
    normed = (
        wide * lax.rsqrt(jnp.mean(wide * wide, axis=-1, keepdims=True) + epsilon) * norm_gain
    ).astype(jnp.bfloat16)
    own_chan = lax.dynamic_slice_in_dim(normed, tp_index * group_width, group_width, 1)
    beside = partner(normed)
    before, after = halo(own_chan)

    pair = lax.dynamic_slice_in_dim(
        lax.all_gather(jnp.concatenate([wk, wv], axis=1), "core", axis=0, tiled=True),
        core * wk.shape[1],
        wk.shape[1],
        1,
    )
    far = spread(pair, "zh")
    far, beside, before, after = lax.optimization_barrier((far, beside, before, after))
    whole = jnp.swapaxes(
        lax.all_gather(far, ("zm", "zl"), axis=0), 0, 1
    ).reshape(model, -1)

    def project(x):
        return jnp.dot(x, whole, preferred_element_type=jnp.float32).astype(jnp.bfloat16)

    ours, theirs = project(normed), project(beside)
    first = jnp.where(core == 0, ours, theirs)
    second = jnp.where(core == 0, theirs, ours)
    own = lax.all_gather(jnp.concatenate([first, second], axis=0), "zh", axis=0, tiled=True)
    mid = own.shape[0] // 2
    mine = [
        own,
        shifted(own, Z, 1),
        shifted(own, Z, -1),
        shifted(own[:mid], Z, 2),
        shifted(own[mid:], Z, -2),
    ]
    other = [partner(p) for p in mine]

    pooled = pooled_rows(own_chan, before, after, tp_index, sp_index, sp_count)

    late, other[-1] = lax.optimization_barrier((late, other[-1]))
    width = wq.shape[1]
    queries = jnp.dot(
        normed, late[:, :width], preferred_element_type=jnp.float32
    ).astype(jnp.bfloat16)
    head_rows, lse = attend(core.reshape(1), queries, head_gain, map_lambda, mine, other)
    log_totals = lse.reshape(2, local_heads, rows)
    partial = lax.dot_general(
        jnp.concatenate([head_rows, pooled], axis=1),
        late[:, width:],
        (((1,), (1,)), ((), ())),
        preferred_element_type=jnp.float32,
    ).astype(jnp.bfloat16)
    tp = lax.axis_size("tp")
    arrived = lax.all_to_all(
        partial.reshape(tp, rows // tp, -1), "tp", split_axis=0, concat_axis=0, tiled=True
    )
    return arrived.astype(jnp.float32).sum(axis=0).astype(jnp.bfloat16), log_totals


def solution(mesh):
    grp, sp, tp = (mesh.shape[a] for a in ("grp", "sp", "tp"))
    fine = Mesh(
        mesh.devices.reshape(grp, sp // (4 * CORES), 2, 2, CORES, tp), ("grp", *SP, "tp")
    )
    placed = (
        P(("grp", *SP), None),
        P(),
        P(SP, "tp"),
        P(SP, "tp"),
        P(SP, "tp"),
        P("tp"),
        P("tp", None),
        P("tp", SP),
        P("tp", SP),
    )
    return jax.shard_map(
        on_device,
        mesh=fine,
        in_specs=placed,
        out_specs=(P(("grp", *SP, "tp"), None), P(None, "tp", ("grp", *SP))),
        check_vma=False,
    )
```

```python
import functools
import math

import jax
import jax.numpy as jnp
from jax import lax
from jax.experimental import pallas as pl
from jax.experimental.pallas import tpu as pltpu
from jax.sharding import Mesh, PartitionSpec as P

HD = 64
VD = 128
POOL_SPAN = 16
CORES = 2
epsilon = 1e-06
LOG2E = math.log2(math.e)
CHUNK = 2560
TILE = 256
ONES = 16
SP = ("zh", "zm", "zl", "core")
Z = ("zh", "zm", "zl")
SWAP = [(0, 1), (1, 0)]


def mixer_kernel(kv_count, place_ref, x_ref, pooled_ref, gain_ref, lam_ref, late_ref, *refs):
    mine, refs = refs[:kv_count], refs[kv_count:]
    other, refs = refs[:kv_count], refs[kv_count:]
    out_ref, lse_ref, qT, qrows, m_s, acc, k_all, v_all, wq, wo, sources, sems = refs
    n, width = pooled_ref.shape
    get_wq = pltpu.make_async_copy(late_ref.at[:, :width], wq, sems.at[0])
    get_wo = pltpu.make_async_copy(late_ref.at[:, width:], wo, sems.at[1])
    get_wq.start()
    get_wo.start()
    heads = width // VD
    half = heads * n
    tiles = 2 * half // TILE

    def fill(keys, values):
        at = 0
        for k, v in zip(keys, values):
            k_all[at : at + k.shape[0], :] = k[...]
            v_all[at : at + v.shape[0], :] = v[...]
            at += k.shape[0]

    @pl.when(place_ref[0] == 0)
    def _():
        fill(mine, other)

    @pl.when(place_ref[0] != 0)
    def _():
        fill(other, mine)

    get_wq.wait()
    queries = jnp.dot(x_ref[...], wq[...], preferred_element_type=jnp.float32)
    queries = queries.astype(jnp.bfloat16).astype(jnp.float32) * (HD**-0.5 * LOG2E)
    lane = lax.broadcasted_iota(jnp.int32, (n, VD), 1)
    for g in range(heads):
        for m in range(2):
            part = jnp.where((lane < HD) == (m == 0), queries[:, g * VD : (g + 1) * VD], 0.0)
            hi = part.astype(jnp.bfloat16)
            lo = (part - hi.astype(jnp.float32)).astype(jnp.bfloat16)
            row = m * half + g * n
            qrows[row : row + n, :VD] = hi
            qrows[row : row + n, VD:] = lo
    for j in range(tiles):
        qT[:, j * TILE : (j + 1) * TILE] = qrows[j * TILE : (j + 1) * TILE, :].T
    m_s[...] = jnp.full(m_s.shape, -jnp.inf, jnp.float32)
    acc[...] = jnp.zeros_like(acc)

    def block(i, carry):
        rows = pl.ds(pl.multiple_of(i * CHUNK, CHUNK), CHUNK)
        keys = k_all[rows, :]
        both = jnp.concatenate([keys, keys], axis=1)
        values_t = jnp.concatenate(
            [v_all[rows, :].T, jnp.ones((ONES, CHUNK), jnp.bfloat16)], axis=0
        )
        scores, weights = {}, {}

        def score(j):
            scores[j] = jnp.dot(
                both, qT[:, j * TILE : (j + 1) * TILE], preferred_element_type=jnp.float32
            )

        def soften(j):
            cols = slice(j * TILE, (j + 1) * TILE)
            s = scores.pop(j)
            m_old = m_s[:, cols]
            m_new = jnp.maximum(m_old, jnp.max(s, axis=0, keepdims=True))
            p = jnp.exp2(s - m_new)
            alpha = jnp.exp2(m_old - m_new)
            m_s[:, cols] = m_new
            weights[j] = (alpha, p.astype(jnp.bfloat16))

        def mix(j):
            cols = slice(j * TILE, (j + 1) * TILE)
            alpha, p = weights.pop(j)
            acc[:, cols] = acc[:, cols] * alpha + jnp.dot(
                values_t, p, preferred_element_type=jnp.float32
            )

        for t in range(tiles + 3):
            if t < tiles:
                score(t)
            if 1 <= t <= tiles:
                soften(t - 1)
            if t >= 3:
                mix(t - 3)
        return carry

    lax.fori_loop(0, k_all.shape[0] // CHUNK, block, 0)

    totals = acc[VD : VD + 1, :]
    lse_ref[...] = m_s[...] * (1.0 / LOG2E) + jnp.log(totals)
    reads = acc[:VD, :] / totals
    contrast = reads[:, :half] - lam_ref[...] * reads[:, half:]
    scaled = contrast * lax.rsqrt(jnp.mean(contrast * contrast, axis=0, keepdims=True) + epsilon)
    rows = scaled.T
    for g in range(heads):
        sources[:, g * VD : (g + 1) * VD] = (
            rows[g * n : (g + 1) * n, :] * gain_ref[g : g + 1, :]
        ).astype(jnp.bfloat16)
    sources[:, width:] = pooled_ref[...]
    get_wo.wait()
    step = 512
    for c in range(0, wo.shape[0], step):
        out_ref[:, c : c + step] = lax.dot_general(
            sources[...],
            wo[c : c + step, :],
            (((1,), (1,)), ((), ())),
            preferred_element_type=jnp.float32,
        ).astype(jnp.bfloat16)


def mixer(place, x, pooled, gain, lam, late, mine, other):
    n, width = pooled.shape
    model = x.shape[1]
    cols = 2 * (width // VD) * n
    keys = sum(p.shape[0] for p in mine)
    vmem = pl.BlockSpec(memory_space=pltpu.VMEM)
    return pl.pallas_call(
        functools.partial(mixer_kernel, len(mine)),
        out_shape=(
            jax.ShapeDtypeStruct((n, late.shape[0]), jnp.bfloat16),
            jax.ShapeDtypeStruct((1, cols), jnp.float32),
        ),
        in_specs=[pl.BlockSpec(memory_space=pltpu.SMEM)]
        + [vmem] * 4
        + [pl.BlockSpec(memory_space=pl.ANY)]
        + [vmem] * (2 * len(mine)),
        out_specs=(vmem, vmem),
        scratch_shapes=[
            pltpu.VMEM((2 * VD, cols), jnp.bfloat16),
            pltpu.VMEM((cols, 2 * VD), jnp.bfloat16),
            pltpu.VMEM((1, cols), jnp.float32),
            pltpu.VMEM((VD + ONES, cols), jnp.float32),
            pltpu.VMEM((keys, VD), jnp.bfloat16),
            pltpu.VMEM((keys, VD), jnp.bfloat16),
            pltpu.VMEM((model, width), jnp.bfloat16),
            pltpu.VMEM((late.shape[0], late.shape[1] - width), jnp.bfloat16),
            pltpu.VMEM((n, late.shape[1] - width), jnp.bfloat16),
            pltpu.SemaphoreType.DMA((2,)),
        ],
        cost_estimate=pl.CostEstimate(
            flops=2 * cols * keys * 3 * VD, bytes_accessed=keys * 4 * VD, transcendentals=cols * keys
        ),
        name="mixer",
    )(place, x, pooled, gain, jnp.repeat(lam, n)[None, :], late, *mine, *other)


def spread(x, axis):
    count = lax.axis_size(axis)
    return lax.all_to_all(jnp.broadcast_to(x[None], (count, *x.shape)), axis, 0, 0, tiled=True)


def shifted(x, axis, by):
    count = lax.axis_size(axis)
    return lax.ppermute(x, axis, [((i + by) % count, i) for i in range(count)])


def partner(x):
    return lax.ppermute(x, "core", SWAP)


def halo(own):
    reach = POOL_SPAN // 2
    ends = math.prod(lax.axis_size(a) for a in SP) - 1
    before = lax.ppermute(own[own.shape[0] - reach :], SP, [(i, i + 1) for i in range(ends)])
    after = lax.ppermute(own[:reach], SP, [(i + 1, i) for i in range(ends)])
    return before, after


def pooled_rows(own, before, after, tp_index, sp_index, sp_count):
    rows = own.shape[0]
    reach = POOL_SPAN // 2
    padded = jnp.concatenate([before, own, after], axis=0)
    window = jnp.left_shift(jnp.int32(2), tp_index)
    half = window // 2
    row = lax.broadcasted_iota(jnp.int32, (rows, rows + 2 * reach), 0)
    col = lax.broadcasted_iota(jnp.int32, (rows, rows + 2 * reach), 1) - reach
    band = ((col >= row - half) & (col < row + window - half)).astype(jnp.bfloat16)
    sums = jnp.dot(band, padded, preferred_element_type=jnp.float32)
    seq_len = rows * sp_count
    position = sp_index * rows + jnp.arange(rows, dtype=jnp.int32)
    lower = jnp.clip(position - half, 0, seq_len)
    upper = jnp.clip(position + window - half, 0, seq_len)
    counts = (upper - lower).astype(jnp.float32)[:, None]
    return (sums / counts - own.astype(jnp.float32)).astype(jnp.bfloat16)


def on_device(tokens, norm_gain, wq, wk, wv, map_lambda, head_gain, ao, po):
    zh, zm, zl = (lax.axis_size(a) for a in Z)
    sp_count = zh * zm * zl * CORES
    sp_index, tp_index = lax.axis_index(SP), lax.axis_index("tp")
    core = lax.axis_index("core")
    rows, model = tokens.shape
    local_heads = map_lambda.shape[0]
    group_width = po.shape[0]

    late = jnp.concatenate([wq, ao.T, po.T], axis=1)
    late, wk, wv = lax.optimization_barrier((late, wk, wv))
    late = lax.all_gather(late, SP, axis=0, tiled=True)

    wide = tokens.astype(jnp.float32)
    normed = (
        wide * lax.rsqrt(jnp.mean(wide * wide, axis=-1, keepdims=True) + epsilon) * norm_gain
    ).astype(jnp.bfloat16)
    own_chan = lax.dynamic_slice_in_dim(normed, tp_index * group_width, group_width, 1)
    beside = partner(normed)
    before, after = halo(own_chan)

    pair = lax.dynamic_slice_in_dim(
        lax.all_gather(jnp.concatenate([wk, wv], axis=1), "core", axis=0, tiled=True),
        core * wk.shape[1],
        wk.shape[1],
        1,
    )
    far = spread(pair, "zh")
    far, beside, before, after = lax.optimization_barrier((far, beside, before, after))
    whole = jnp.swapaxes(
        lax.all_gather(far, ("zm", "zl"), axis=0), 0, 1
    ).reshape(model, -1)

    def project(x):
        return jnp.dot(x, whole, preferred_element_type=jnp.float32).astype(jnp.bfloat16)

    ours, theirs = project(normed), project(beside)
    first = jnp.where(core == 0, ours, theirs)
    second = jnp.where(core == 0, theirs, ours)
    own = lax.all_gather(jnp.concatenate([first, second], axis=0), "zh", axis=0, tiled=True)
    mid = own.shape[0] // 2
    low, high, kept = lax.optimization_barrier((own[:mid], own[mid:], own))
    mine = [
        own,
        shifted(own, Z, 1),
        shifted(own, Z, -1),
        shifted(low, Z, 2),
        shifted(high, Z, -2),
    ]
    other = [partner(p) for p in (kept, *mine[1:])]

    pooled = pooled_rows(own_chan, before, after, tp_index, sp_index, sp_count)

    late, other[-1] = lax.optimization_barrier((late, other[-1]))
    partial, lse = mixer(
        core.reshape(1), normed, pooled, head_gain, map_lambda, late, mine, other
    )
    log_totals = lse.reshape(2, local_heads, rows)
    tp = lax.axis_size("tp")
    arrived = lax.all_to_all(
        partial.reshape(tp, rows // tp, -1), "tp", split_axis=0, concat_axis=0, tiled=True
    )
    return arrived.astype(jnp.float32).sum(axis=0).astype(jnp.bfloat16), log_totals


def solution(mesh):
    grp, sp, tp = (mesh.shape[a] for a in ("grp", "sp", "tp"))
    fine = Mesh(
        mesh.devices.reshape(grp, sp // (4 * CORES), 2, 2, CORES, tp), ("grp", *SP, "tp")
    )
    placed = (
        P(("grp", *SP), None),
        P(),
        P(SP, "tp"),
        P(SP, "tp"),
        P(SP, "tp"),
        P("tp"),
        P("tp", None),
        P("tp", SP),
        P("tp", SP),
    )
    return jax.shard_map(
        on_device,
        mesh=fine,
        in_specs=placed,
        out_specs=(P(("grp", *SP, "tp"), None), P(None, "tp", ("grp", *SP))),
        check_vma=False,
    )
```

```python
import functools
import math

import jax
import jax.numpy as jnp
from jax import lax
from jax.experimental import pallas as pl
from jax.experimental.pallas import tpu as pltpu
from jax.sharding import Mesh, PartitionSpec as P

HD = 64
VD = 128
POOL_SPAN = 16
CORES = 2
epsilon = 1e-06
LOG2E = math.log2(math.e)
CHUNK = 2560
TILE = 256
ONES = 16
SP = ("zh", "zm", "zl", "core")
Z = ("zh", "zm", "zl")
SWAP = [(0, 1), (1, 0)]


def mixer_kernel(kv_count, place_ref, x_ref, pooled_ref, gain_ref, lam_ref, late_ref, *refs):
    mine, refs = refs[:kv_count], refs[kv_count:]
    other, refs = refs[:kv_count], refs[kv_count:]
    out_ref, lse_ref, qT, qrows, m_s, acc, k_all, v_all, wq, wo, sources, sems = refs
    n, width = pooled_ref.shape
    get_wq = pltpu.make_async_copy(late_ref.at[:, :width], wq, sems.at[0])
    get_wo = pltpu.make_async_copy(late_ref.at[:, width:], wo, sems.at[1])
    get_wq.start()
    get_wo.start()
    heads = width // VD
    half = heads * n
    tiles = 2 * half // TILE

    def fill(keys, values):
        at = 0
        for k, v in zip(keys, values):
            k_all[at : at + k.shape[0], :] = k[...]
            v_all[at : at + v.shape[0], :] = v[...]
            at += k.shape[0]

    @pl.when(place_ref[0] == 0)
    def _():
        fill(mine, other)

    @pl.when(place_ref[0] != 0)
    def _():
        fill(other, mine)

    get_wq.wait()
    queries = jnp.dot(x_ref[...], wq[...], preferred_element_type=jnp.float32)
    queries = queries.astype(jnp.bfloat16).astype(jnp.float32) * (HD**-0.5 * LOG2E)
    lane = lax.broadcasted_iota(jnp.int32, (n, VD), 1)
    for g in range(heads):
        for m in range(2):
            part = jnp.where((lane < HD) == (m == 0), queries[:, g * VD : (g + 1) * VD], 0.0)
            hi = part.astype(jnp.bfloat16)
            lo = (part - hi.astype(jnp.float32)).astype(jnp.bfloat16)
            row = m * half + g * n
            qrows[row : row + n, :VD] = hi
            qrows[row : row + n, VD:] = lo
    for j in range(tiles):
        qT[:, j * TILE : (j + 1) * TILE] = qrows[j * TILE : (j + 1) * TILE, :].T
    m_s[...] = jnp.full(m_s.shape, -jnp.inf, jnp.float32)
    acc[...] = jnp.zeros_like(acc)

    def block(i, carry):
        rows = pl.ds(pl.multiple_of(i * CHUNK, CHUNK), CHUNK)
        keys = k_all[rows, :]
        both = jnp.concatenate([keys, keys], axis=1)
        values_t = jnp.concatenate(
            [v_all[rows, :].T, jnp.ones((ONES, CHUNK), jnp.bfloat16)], axis=0
        )
        scores, weights = {}, {}

        def score(j):
            scores[j] = jnp.dot(
                both, qT[:, j * TILE : (j + 1) * TILE], preferred_element_type=jnp.float32
            )

        def soften(j):
            cols = slice(j * TILE, (j + 1) * TILE)
            s = scores.pop(j)
            m_old = m_s[:, cols]
            m_new = jnp.maximum(m_old, jnp.max(s, axis=0, keepdims=True))
            p = jnp.exp2(s - m_new)
            alpha = jnp.exp2(m_old - m_new)
            m_s[:, cols] = m_new
            weights[j] = (alpha, p.astype(jnp.bfloat16))

        def mix(j):
            cols = slice(j * TILE, (j + 1) * TILE)
            alpha, p = weights.pop(j)
            acc[:, cols] = acc[:, cols] * alpha + jnp.dot(
                values_t, p, preferred_element_type=jnp.float32
            )

        for t in range(tiles + 3):
            if t < tiles:
                score(t)
            if 1 <= t <= tiles:
                soften(t - 1)
            if t >= 3:
                mix(t - 3)
        return carry

    lax.fori_loop(0, k_all.shape[0] // CHUNK, block, 0)

    totals = acc[VD : VD + 1, :]
    lse_ref[...] = m_s[...] * (1.0 / LOG2E) + jnp.log(totals)
    reads = acc[:VD, :] / totals
    contrast = reads[:, :half] - lam_ref[...] * reads[:, half:]
    scaled = contrast * lax.rsqrt(jnp.mean(contrast * contrast, axis=0, keepdims=True) + epsilon)
    rows = scaled.T
    for g in range(heads):
        sources[:, g * VD : (g + 1) * VD] = (
            rows[g * n : (g + 1) * n, :] * gain_ref[g : g + 1, :]
        ).astype(jnp.bfloat16)
    sources[:, width:] = pooled_ref[...]
    get_wo.wait()
    step = 512
    for c in range(0, wo.shape[0], step):
        out_ref[:, c : c + step] = lax.dot_general(
            sources[...],
            wo[c : c + step, :],
            (((1,), (1,)), ((), ())),
            preferred_element_type=jnp.float32,
        ).astype(jnp.bfloat16)


def mixer(place, x, pooled, gain, lam, late, mine, other):
    n, width = pooled.shape
    model = x.shape[1]
    cols = 2 * (width // VD) * n
    keys = sum(p.shape[0] for p in mine)
    vmem = pl.BlockSpec(memory_space=pltpu.VMEM)
    return pl.pallas_call(
        functools.partial(mixer_kernel, len(mine)),
        out_shape=(
            jax.ShapeDtypeStruct((n, late.shape[0]), jnp.bfloat16),
            jax.ShapeDtypeStruct((1, cols), jnp.float32),
        ),
        in_specs=[pl.BlockSpec(memory_space=pltpu.SMEM)]
        + [vmem] * 4
        + [pl.BlockSpec(memory_space=pl.ANY)]
        + [vmem] * (2 * len(mine)),
        out_specs=(vmem, vmem),
        scratch_shapes=[
            pltpu.VMEM((2 * VD, cols), jnp.bfloat16),
            pltpu.VMEM((cols, 2 * VD), jnp.bfloat16),
            pltpu.VMEM((1, cols), jnp.float32),
            pltpu.VMEM((VD + ONES, cols), jnp.float32),
            pltpu.VMEM((keys, VD), jnp.bfloat16),
            pltpu.VMEM((keys, VD), jnp.bfloat16),
            pltpu.VMEM((model, width), jnp.bfloat16),
            pltpu.VMEM((late.shape[0], late.shape[1] - width), jnp.bfloat16),
            pltpu.VMEM((n, late.shape[1] - width), jnp.bfloat16),
            pltpu.SemaphoreType.DMA((2,)),
        ],
        cost_estimate=pl.CostEstimate(
            flops=2 * cols * keys * 3 * VD, bytes_accessed=keys * 4 * VD, transcendentals=cols * keys
        ),
        name="mixer",
    )(place, x, pooled, gain, jnp.repeat(lam, n)[None, :], late, *mine, *other)


def spread(x, axis):
    count = lax.axis_size(axis)
    return lax.all_to_all(jnp.broadcast_to(x[None], (count, *x.shape)), axis, 0, 0, tiled=True)


def shifted(x, axis, by):
    count = lax.axis_size(axis)
    return lax.ppermute(x, axis, [((i + by) % count, i) for i in range(count)])


def partner(x):
    return lax.ppermute(x, "core", SWAP)


def halo(own):
    reach = POOL_SPAN // 2
    ends = math.prod(lax.axis_size(a) for a in SP) - 1
    before = lax.ppermute(own[own.shape[0] - reach :], SP, [(i, i + 1) for i in range(ends)])
    after = lax.ppermute(own[:reach], SP, [(i + 1, i) for i in range(ends)])
    return before, after


def pooled_rows(own, before, after, tp_index, sp_index, sp_count):
    rows = own.shape[0]
    reach = POOL_SPAN // 2
    padded = jnp.concatenate([before, own, after], axis=0)
    window = jnp.left_shift(jnp.int32(2), tp_index)
    half = window // 2
    row = lax.broadcasted_iota(jnp.int32, (rows, rows + 2 * reach), 0)
    col = lax.broadcasted_iota(jnp.int32, (rows, rows + 2 * reach), 1) - reach
    band = ((col >= row - half) & (col < row + window - half)).astype(jnp.bfloat16)
    sums = jnp.dot(band, padded, preferred_element_type=jnp.float32)
    seq_len = rows * sp_count
    position = sp_index * rows + jnp.arange(rows, dtype=jnp.int32)
    lower = jnp.clip(position - half, 0, seq_len)
    upper = jnp.clip(position + window - half, 0, seq_len)
    counts = (upper - lower).astype(jnp.float32)[:, None]
    return (sums / counts - own.astype(jnp.float32)).astype(jnp.bfloat16)


def on_device(tokens, norm_gain, wq, wk, wv, map_lambda, head_gain, ao, po):
    zh, zm, zl = (lax.axis_size(a) for a in Z)
    sp_count = zh * zm * zl * CORES
    sp_index, tp_index = lax.axis_index(SP), lax.axis_index("tp")
    core = lax.axis_index("core")
    rows, model = tokens.shape
    local_heads = map_lambda.shape[0]
    group_width = po.shape[0]

    late = jnp.concatenate([wq, ao.T, po.T], axis=1)
    late, wk, wv = lax.optimization_barrier((late, wk, wv))
    late = lax.all_gather(late, SP, axis=0, tiled=True)

    wide = tokens.astype(jnp.float32)
    normed = (
        wide * lax.rsqrt(jnp.mean(wide * wide, axis=-1, keepdims=True) + epsilon) * norm_gain
    ).astype(jnp.bfloat16)
    own_chan = lax.dynamic_slice_in_dim(normed, tp_index * group_width, group_width, 1)
    beside = partner(normed)
    before, after = halo(own_chan)

    pair = lax.dynamic_slice_in_dim(
        lax.all_gather(jnp.concatenate([wk, wv], axis=1), "core", axis=0, tiled=True),
        core * wk.shape[1],
        wk.shape[1],
        1,
    )
    far = spread(pair, "zh")
    far, beside, before, after = lax.optimization_barrier((far, beside, before, after))
    whole = jnp.swapaxes(
        lax.all_gather(far, ("zm", "zl"), axis=0), 0, 1
    ).reshape(model, -1)

    def project(x):
        return jnp.dot(x, whole, preferred_element_type=jnp.float32).astype(jnp.bfloat16)

    ours, theirs = project(normed), project(beside)
    first = jnp.where(core == 0, ours, theirs)
    second = jnp.where(core == 0, theirs, ours)
    own = lax.all_gather(jnp.concatenate([first, second], axis=0), "zh", axis=0, tiled=True)
    mid = own.shape[0] // 2
    low, high, kept = lax.optimization_barrier((own[:mid], own[mid:], own))
    mine = [
        own,
        shifted(own, Z, 1),
        shifted(own, Z, -1),
        shifted(low, Z, 2),
        shifted(high, Z, -2),
    ]
    kept, mine[1] = lax.optimization_barrier((kept, mine[1]))
    other = [partner(p) for p in (kept, *mine[1:])]

    pooled = pooled_rows(own_chan, before, after, tp_index, sp_index, sp_count)

    late, other[-1] = lax.optimization_barrier((late, other[-1]))
    partial, lse = mixer(
        core.reshape(1), normed, pooled, head_gain, map_lambda, late, mine, other
    )
    log_totals = lse.reshape(2, local_heads, rows)
    tp = lax.axis_size("tp")
    arrived = lax.all_to_all(
        partial.reshape(tp, rows // tp, -1), "tp", split_axis=0, concat_axis=0, tiled=True
    )
    return arrived.astype(jnp.float32).sum(axis=0).astype(jnp.bfloat16), log_totals


def solution(mesh):
    grp, sp, tp = (mesh.shape[a] for a in ("grp", "sp", "tp"))
    fine = Mesh(
        mesh.devices.reshape(grp, sp // (4 * CORES), 2, 2, CORES, tp), ("grp", *SP, "tp")
    )
    placed = (
        P(("grp", *SP), None),
        P(),
        P(SP, "tp"),
        P(SP, "tp"),
        P(SP, "tp"),
        P("tp"),
        P("tp", None),
        P("tp", SP),
        P("tp", SP),
    )
    return jax.shard_map(
        on_device,
        mesh=fine,
        in_specs=placed,
        out_specs=(P(("grp", *SP, "tp"), None), P(None, "tp", ("grp", *SP))),
        check_vma=False,
    )
```
